32 devices in a mesh: sp: 8 (over z, core), tp: 4 (over y, x).
Axes of the slice: x: 2, y: 2, z: 4, core: 2. Of those that a mesh axis runs over, the one named last changes fastest.
Arguments:
- tokens: bfloat16 [8192, 4096], P('sp', 'tp'), may hold values from -6 to 6
- key_weight: bfloat16 [4096, 1024], P(None, 'tp'), may hold values from -0.005859375 to 0.005859375
- value_weight: bfloat16 [4096, 2048], P(None, 'tp'), may hold values from -0.09375 to 0.09375
- decay_weight: bfloat16 [2, 4096, 1024], P(None, None, 'tp'), may hold values from -0.09375 to 0.09375
- decay_bias: float32 [2, 1024], P(None, 'tp')
- decay_shift: float32 [8192, 16], P('sp', 'tp'), may hold values from -0.65 to 0
- new_query: bfloat16 [16, 64], P('tp'), may hold values from -6 to 6
- new_key: bfloat16 [16, 64], P('tp'), may hold values from -6 to 6
- new_value: bfloat16 [16, 128], P('tp'), may hold values from -6 to 6
- out_gain: float32 [128], replicated, may hold values from 0.1 to 1.9
Outputs:
- state_cache: bfloat16 [2, 16, 64, 128], P(None, 'tp', 'sp')
- decode_read: bfloat16 [16, 128], P('tp')
The draws below stay inside these ranges and needn't reach their ends.
All inputs are finite; a program needn't handle non-finite values.
Results may differ from the reference program's by a relative error of at most 0.0039.
Values may be sent and summed in bfloat16 or wider, within the bound.
A program may use at most 64 MiB of HBM per device.

```python
from functools import partial
import jax
import jax.numpy as jnp
from jax import lax

D = 4096
H = 16
DK = 64
DV = 128
TOK_DEV = 1024
LEN = 8192
N_SP = 8


def draw_decay_bias(key, part):
    key_slow, key_low, key_high = jax.random.split(jax.random.fold_in(key, 11), 3)
    share = 0.5
    slow_heads = jax.random.uniform(key_slow, (2, H, 1)) < share
    slow_value = jnp.log(2.0 * TOK_DEV) + jax.random.uniform(key_high, (2, H, DK), minval=-0.5, maxval=0.5)
    fast_value = jax.random.uniform(key_low, (2, H, DK), minval=-1.0, maxval=1.0)
    return jnp.where(slow_heads, slow_value, fast_value).reshape(2, H * DK).astype(jnp.float32)


def draw_decay_shift(key, part):
    key_rate, key_where, key_gap, key_depth = jax.random.split(jax.random.fold_in(key, 23), 4)
    seg_count = LEN // TOK_DEV
    rate = jnp.exp(jax.random.uniform(key_rate, (seg_count, 1, 1), minval=0.0, maxval=jnp.log(4.0)))
    base = jnp.broadcast_to(-0.25 * rate / LEN, (seg_count, TOK_DEV, H)).reshape(LEN, H)
    leading_location = jax.random.randint(key_where, (), 0, LEN)
    gap = jax.random.randint(key_gap, (), 1, LEN)
    trailing_location = (leading_location + gap) % LEN
    spike_location = jnp.stack([leading_location, trailing_location]).astype(jnp.int32)
    sequence_indices = jnp.arange(LEN, dtype=jnp.int32)[:, None]
    agreeing_tally = jnp.sum((sequence_indices == spike_location[None, :]).astype(jnp.float32), axis=1, keepdims=True)
    depth = jnp.log(jax.random.uniform(key_depth, (1, H), minval=0.55, maxval=0.8))
    return (base + agreeing_tally * depth).astype(jnp.float32)


def steps_of(own_key, dims, cuts, low, top_value):
    factor_of, own = 1.0, jax.random.fold_in(own_key, 6)
    for position, shards_of in cuts:
        draws = jnp.exp(jax.random.uniform(jax.random.fold_in(own, position), (shards_of,), jnp.float32, low / len(cuts), top_value / len(cuts)))
        factor_of = factor_of * jnp.repeat(draws, dims[position] // shards_of).reshape([-1 if axis == position else 1 for axis in range(len(dims))])
    return factor_of


def normal_values(own_key, shape, spread, bound, cuts=(), kind=jnp.bfloat16):
    loudness = steps_of(own_key, shape, cuts, -0.22, 0.18) if cuts else 1.0
    entries = jax.random.normal(own_key, shape, jnp.float32) * spread * loudness
    return jnp.minimum(jnp.maximum(entries, -bound), bound).astype(kind)


def setup_inputs(seed: int = 0) -> dict:
    splits = jax.random.split(jax.random.key(seed), 11)
    return {
        "tokens": normal_values(splits[0], (LEN, D), 1.0, 6.0, ((0, 8), (1, 4))),
        "key_weight": normal_values(splits[1], (D, H * DK), (D * 256) ** -0.5, 0.005859375, ((1, 4),)),
        "value_weight": normal_values(splits[2], (D, H * DV), D ** -0.5, 0.09375, ((1, 4),)),
        "decay_weight": normal_values(splits[3], (2, D, H * DK), D ** -0.5, 0.09375, ((2, 4),)),
        "decay_bias": draw_decay_bias(jax.random.fold_in(splits[10], 71), 0),
        "decay_shift": draw_decay_shift(jax.random.fold_in(splits[10], 71), 0),
        "new_query": normal_values(splits[6], (H, DK), 1.0, 6.0, ((0, 4),)),
        "new_key": normal_values(splits[7], (H, DK), 1.0, 6.0, ((0, 4),)),
        "new_value": normal_values(splits[8], (H, DV), 1.0, 6.0, ((0, 4),)),
        "out_gain": jnp.clip(1.0 + 0.18 * jax.random.normal(splits[9], (DV,), jnp.float32), 0.1, 1.9),
    }


gate_norm = 16.0
norm_epsilon = 1e-06

def head_states(tokens, inputs):
    weight_key, weight_value, onward_coefficient_matrix, weight_bwd, forward_bias_terms, reverse_offset_vector, shift_head = inputs
    combined = jnp.concatenate([weight_key, weight_value, onward_coefficient_matrix, weight_bwd], axis=1)
    projected = jnp.dot(tokens, combined, preferred_element_type=jnp.float32)
    key_proj = projected[:, :DK].astype(jnp.bfloat16)
    value_proj = projected[:, DK:DK + DV].astype(jnp.bfloat16)
    fwd_log = jax.nn.log_sigmoid(projected[:, DK + DV:2 * DK + DV] + forward_bias_terms) / gate_norm + shift_head[:, None]
    bwd_log = jax.nn.log_sigmoid(projected[:, 2 * DK + DV:] + reverse_offset_vector) / gate_norm + shift_head[:, None]
    fwd_seg = fwd_log.reshape(N_SP, TOK_DEV, DK)
    bwd_seg = bwd_log.reshape(N_SP, TOK_DEV, DK)
    key_seg = key_proj.reshape(N_SP, TOK_DEV, DK)
    value_seg = value_proj.reshape(N_SP, TOK_DEV, DV).astype(jnp.float32)
    fwd_total = lax.optimization_barrier(jnp.sum(fwd_seg, axis=1))
    bwd_total = lax.optimization_barrier(jnp.sum(bwd_seg, axis=1))
    fwd_inside = fwd_total[:, None, :] - jnp.cumsum(fwd_seg, axis=1)
    bwd_inside = jnp.cumsum(bwd_seg, axis=1) - bwd_seg
    fwd_keys = (key_seg * jnp.exp(fwd_inside)).astype(jnp.bfloat16)
    bwd_keys = (key_seg * jnp.exp(bwd_inside)).astype(jnp.bfloat16)
    fwd_local = jnp.einsum('ntc,ntv->ncv', fwd_keys.astype(jnp.float32), value_seg, precision=lax.Precision.HIGHEST)
    bwd_local = jnp.einsum('ntc,ntv->ncv', bwd_keys.astype(jnp.float32), value_seg, precision=lax.Precision.HIGHEST)
    fwd_later = lax.optimization_barrier(jnp.sum(fwd_total, axis=0))[None, :] - jnp.cumsum(fwd_total, axis=0)
    bwd_earlier = jnp.cumsum(bwd_total, axis=0) - bwd_total
    fwd_state = lax.optimization_barrier(jnp.sum(jnp.exp(fwd_later)[:, :, None] * fwd_local, axis=0))
    bwd_state = lax.optimization_barrier(jnp.sum(jnp.exp(bwd_earlier)[:, :, None] * bwd_local, axis=0))
    return (fwd_state, bwd_state)

def reference(tokens, key_weight, value_weight, decay_weight, decay_bias, decay_shift, new_query, new_key, new_value, out_gain):
    key_heads = key_weight.reshape(D, H, DK).transpose(1, 0, 2)
    value_head_count = value_weight.reshape(D, H, DV).transpose(1, 0, 2)
    fwd_heads = decay_weight[0].reshape(D, H, DK).transpose(1, 0, 2)
    bwd_heads = decay_weight[1].reshape(D, H, DK).transpose(1, 0, 2)
    forward_bias_terms = decay_bias[0].reshape(H, DK)
    reverse_offset_vector = decay_bias[1].reshape(H, DK)
    shift_heads = decay_shift.T
    fwd_states, bwd_states = lax.map(partial(head_states, tokens), (key_heads, value_head_count, fwd_heads, bwd_heads, forward_bias_terms, reverse_offset_vector, shift_heads))
    state_cache = jnp.stack([fwd_states, bwd_states]).astype(jnp.bfloat16)
    query_vec = new_query.astype(jnp.float32)
    raw_read = jnp.einsum('hc,hcv->hv', query_vec, fwd_states + bwd_states, precision=lax.Precision.HIGHEST)
    raw_read = raw_read + lax.optimization_barrier(jnp.sum(query_vec * new_key.astype(jnp.float32), axis=-1, keepdims=True)) * new_value.astype(jnp.float32)
    scaled = raw_read * lax.rsqrt(lax.optimization_barrier(jnp.mean(raw_read * raw_read, axis=-1, keepdims=True)) + norm_epsilon) * out_gain
    return (state_cache, scaled.astype(jnp.bfloat16))
```

```python
import functools

import jax
import jax.numpy as jnp
from jax import lax
from jax.experimental import pallas as pl
from jax.experimental.pallas import tpu as pltpu
from jax.sharding import PartitionSpec as P

DK = 64
DV = 128
CHUNK = 128

gate_norm = 16.0
norm_epsilon = 1e-06

MESH = pl.DeviceIdType.MESH


def flipped(index, bits, d):
    out = index
    for b in bits:
        if d & b:
            out = out + b - 2 * b * lax.rem(lax.div(index, b), 2)
    return out


def kernel(
    n_sp,
    n_tp,
    tokens,
    kw,
    vw,
    dw,
    bias,
    shift,
    query,
    new_key,
    new_value,
    gain,
    state_out,
    read_out,
    tok_buf,
    kw_buf,
    vw_buf,
    dw_buf,
    acc_k,
    acc_v,
    acc_d,
    s_fwd,
    s_bwd,
    tot_own,
    tot_buf,
    st_send,
    st_recv,
    rd_send,
    rd_recv,
    local_sem,
    w_sem,
    own_send_sem,
    relay_send_sem,
    recv_sem,
    tot_send_sem,
    tot_recv_sem,
    st_send_sem,
    st_recv_sem,
    rd_send_sem,
    rd_recv_sem,
):
    sp = lax.axis_index("sp")
    tp = lax.axis_index("tp")
    bits = [1 << i for i in range(n_tp.bit_length() - 1)]
    order = sorted(range(n_tp), key=lambda d: (bin(d).count("1"), d))
    level = [bin(d).count("1") for d in order]
    place = {d: i for i, d in enumerate(order)}
    direct = [i for i in range(n_tp) if level[i] == 1]
    near = sum(1 for lv in level if lv <= 1)

    t_count, feat = tokens.shape
    rows = min(CHUNK, t_count)
    half = rows // 2
    chunks = t_count // rows
    width = kw.shape[1]
    heads = width // DK
    pair = 2 if heads % 2 == 0 else 1
    groups = heads // pair
    lanes = pair * DK
    r_count = DK // n_sp

    local = []
    for i, d in enumerate(order):
        src = pl.ds(pl.multiple_of(flipped(tp, bits, d) * feat, feat), feat)
        dst = pl.ds(i * feat, feat)
        local.append(pltpu.make_async_copy(kw.at[src], kw_buf.at[dst], w_sem.at[i, 0]))
        local.append(pltpu.make_async_copy(vw.at[src], vw_buf.at[dst], w_sem.at[i, 1]))
        for k in range(2):
            local.append(
                pltpu.make_async_copy(dw.at[k, src], dw_buf.at[k, dst], w_sem.at[i, 2 + k])
            )
    local.append(pltpu.make_async_copy(tokens, tok_buf.at[0], local_sem.at[0]))

    barrier = pltpu.get_barrier_semaphore()
    for b in bits:
        pl.semaphore_signal(
            barrier, inc=1, device_id=(sp, flipped(tp, bits, b)), device_id_type=MESH
        )
    for d in range(1, n_sp):
        pl.semaphore_signal(
            barrier, inc=1, device_id=(lax.rem(sp + d, n_sp), tp), device_id_type=MESH
        )
    pl.semaphore_wait(barrier, len(bits) + n_sp - 1)

    def part(c, h):
        if h is None:
            return pl.ds(pl.multiple_of(c * rows, rows), rows)
        return pl.ds(pl.multiple_of(c * rows + h * half, half), half)

    def own_copy(c, j):
        b = bits[j]
        rs = part(c, None)
        return pltpu.make_async_remote_copy(
            src_ref=tokens.at[rs],
            dst_ref=tok_buf.at[place[b], rs],
            send_sem=own_send_sem.at[j, c],
            recv_sem=recv_sem.at[place[b], c, 0],
            device_id=(sp, flipped(tp, bits, b)),
            device_id_type=MESH,
        )

    relays = []
    for d in order[1:]:
        for b in bits:
            if not d & b:
                if b > d:
                    relays.append((d, 0, b))
                if all(b < o for o in bits if d & o):
                    relays.append((d, 1, b))

    def relay_copy(c, n):
        d, h, b = relays[n]
        rs = part(c, h)
        return pltpu.make_async_remote_copy(
            src_ref=tok_buf.at[place[d], rs],
            dst_ref=tok_buf.at[place[d | b], rs],
            send_sem=relay_send_sem.at[n, c],
            recv_sem=recv_sem.at[place[d | b], c, h],
            device_id=(sp, flipped(tp, bits, b)),
            device_id_type=MESH,
        )

    def send_own(c):
        for j in range(len(bits)):
            own_copy(c, j).start()

    def wait_direct(c):
        for j in range(len(bits)):
            own_copy(c, j).wait_recv()

    def relay_level(c, lv):
        for n, (d, h, b) in enumerate(relays):
            if bin(d).count("1") == lv:
                relay_copy(c, n).start()

    def wait_level(c, lv):
        for n, (d, h, b) in enumerate(relays):
            if bin(d | b).count("1") == lv:
                relay_copy(c, n).wait_recv()

    for c in range(min(2, chunks)):
        send_own(c)
    for copy in local:
        copy.start()

    s_fwd[...] = jnp.zeros_like(s_fwd)
    s_bwd[...] = jnp.zeros_like(s_bwd)
    tot_own[...] = jnp.zeros_like(tot_own)

    t_ids = lax.broadcasted_iota(jnp.int32, (rows, 2 * rows), 0)
    s_ids = lax.broadcasted_iota(jnp.int32, (rows, 2 * rows), 1)
    s_ids = jnp.where(s_ids >= rows, s_ids - rows, s_ids)
    after = jnp.where(s_ids > t_ids, 1.0, 0.0).astype(jnp.bfloat16)
    before = jnp.where(s_ids < t_ids, 1.0, 0.0).astype(jnp.bfloat16)
    first_head = lax.broadcasted_iota(jnp.int32, (DV, lanes), 1) < DK
    first_head_rows = lax.broadcasted_iota(jnp.int32, (rows, lanes), 1) < DK

    def dot(a, b):
        return jnp.dot(a, b, preferred_element_type=jnp.float32)

    def product(c, low, high):
        rs = part(c, None)
        x = jnp.concatenate([tok_buf[i, rs, :] for i in range(low, high)], axis=1)
        ws = slice(low * feat, high * feat)
        return (
            dot(x, kw_buf[ws, :]),
            dot(x, vw_buf[ws, :]),
            dot(x, dw_buf[0, ws, :]),
            dot(x, dw_buf[1, ws, :]),
        )

    def begin(c):
        p = lax.rem(c, 2)
        k, v, f, b = product(c, 0, near)
        acc_k[p] = k
        acc_v[p] = v
        acc_d[p, 0] = f
        acc_d[p, 1] = b

    def log_gate(pre, shift_wide):
        return (
            jnp.minimum(pre, 0.0) - jnp.log(1.0 + jnp.exp(-jnp.abs(pre)))
        ) * (1.0 / gate_norm) + shift_wide

    def summed(mask, log):
        hi = log.astype(jnp.bfloat16)
        lo = (log - hi.astype(jnp.float32)).astype(jnp.bfloat16)
        return dot(mask, jnp.concatenate([hi, lo], axis=0))

    def finish(c):
        p = lax.rem(c, 2)
        for lv in range(2, len(bits) + 1):
            wait_level(c, lv)
            relay_level(c, lv)
        k, v, f, b = acc_k[p], acc_v[p], acc_d[p, 0], acc_d[p, 1]
        if near < n_tp:
            more = product(c, near, n_tp)
            k, v, f, b = k + more[0], v + more[1], f + more[2], b + more[3]
        k = k.astype(jnp.bfloat16).astype(jnp.float32)
        v = v.astype(jnp.bfloat16)
        sh = shift[part(c, None), :]
        wide = []
        for g in range(groups):
            one = jnp.broadcast_to(sh[:, g * pair : g * pair + 1], (rows, lanes))
            if pair == 2:
                two = jnp.broadcast_to(sh[:, g * pair + 1 : g * pair + 2], (rows, lanes))
                one = jnp.where(first_head_rows, one, two)
            wide.append(one)
        shift_wide = wide[0] if groups == 1 else jnp.concatenate(wide, axis=1)
        f_log = log_gate(f + bias[0:1, :], shift_wide)
        b_log = log_gate(b + bias[1:2, :], shift_wide)
        f_total = jnp.sum(f_log, axis=0, keepdims=True)
        b_total = jnp.sum(b_log, axis=0, keepdims=True)
        f_keys = (k * jnp.exp(summed(after, f_log))).astype(jnp.bfloat16)
        b_keys = (k * jnp.exp(summed(before, b_log) + tot_own[1:2, :])).astype(jnp.bfloat16)
        f_scale = jnp.exp(f_total)
        tot_own[0:1, :] += f_total
        tot_own[1:2, :] += b_total

        def outer(v_group, keys):
            r = lax.dot_general(
                v_group, keys, (((0,), (0,)), ((), ())), preferred_element_type=jnp.float32
            )
            return jnp.where(first_head, r[:DV], r[DV:]) if pair == 2 else r

        for g in range(groups):
            cs = slice(g * lanes, (g + 1) * lanes)
            v_group = v[:, g * pair * DV : (g + 1) * pair * DV]
            s_fwd[:, cs] = s_fwd[:, cs] * f_scale[:, cs] + outer(v_group, f_keys[:, cs])
            s_bwd[:, cs] += outer(v_group, b_keys[:, cs])

    for copy in local:
        copy.wait()

    def step(c, carry):
        wait_direct(c)
        relay_level(c, 1)

        @pl.when(c + 2 < chunks)
        def _():
            send_own(c + 2)

        begin(c)

        @pl.when(c > 0)
        def _():
            finish(c - 1)

        return carry

    lax.fori_loop(0, chunks, step, 0)
    finish(chunks - 1)

    def peer(d):
        return lax.rem(sp + d, n_sp)

    def total_copy(d):
        return pltpu.make_async_remote_copy(
            src_ref=tot_own,
            dst_ref=tot_buf.at[sp],
            send_sem=tot_send_sem.at[d],
            recv_sem=tot_recv_sem.at[sp],
            device_id=(peer(d), tp),
            device_id_type=MESH,
        )

    for d in range(1, n_sp):
        total_copy(d).start()
    later = jnp.zeros((1, width), jnp.float32)
    earlier = jnp.zeros((1, width), jnp.float32)
    for d in range(1, n_sp):
        src = peer(d)
        pltpu.make_async_remote_copy(
            src_ref=tot_own,
            dst_ref=tot_buf.at[src],
            send_sem=tot_send_sem.at[d],
            recv_sem=tot_recv_sem.at[src],
            device_id=(src, tp),
            device_id_type=MESH,
        ).wait_recv()
        got = tot_buf[src]
        later += jnp.where(src > sp, got[0:1, :], 0.0)
        earlier += jnp.where(src < sp, got[1:2, :], 0.0)

    def upright(s):
        tiles = [s[:, g * lanes : (g + 1) * lanes].T for g in range(groups)]
        return tiles[0] if groups == 1 else jnp.concatenate(tiles, axis=0)

    w_fwd = upright(s_fwd[...] * jnp.exp(later))
    w_bwd = upright(s_bwd[...] * jnp.exp(earlier))
    for r in range(n_sp):
        for h in range(heads):
            rs = slice(h * DK + r * r_count, h * DK + (r + 1) * r_count)
            st_send[r, 0, h] = w_fwd[rs]
            st_send[r, 1, h] = w_bwd[rs]

    def state_copy(dst, slot, d):
        return pltpu.make_async_remote_copy(
            src_ref=st_send.at[dst],
            dst_ref=st_recv.at[slot],
            send_sem=st_send_sem.at[d],
            recv_sem=st_recv_sem.at[slot],
            device_id=(dst, tp),
            device_id_type=MESH,
        )

    def read_copy(dst, slot, d):
        return pltpu.make_async_remote_copy(
            src_ref=rd_send,
            dst_ref=rd_recv.at[slot],
            send_sem=rd_send_sem.at[d],
            recv_sem=rd_recv_sem.at[slot],
            device_id=(dst, tp),
            device_id_type=MESH,
        )

    for d in range(1, n_sp):
        state_copy(peer(d), sp, d).start()

    q = query[...].astype(jnp.float32)
    both = w_fwd + w_bwd
    head_ids = lax.broadcasted_iota(jnp.int32, (heads, DV), 0)
    read = jnp.zeros((heads, DV), jnp.float32)
    for h in range(heads):
        one = jnp.dot(
            q,
            both[h * DK : (h + 1) * DK],
            precision=lax.Precision.HIGHEST,
            preferred_element_type=jnp.float32,
        )
        read = jnp.where(head_ids == h, one, read)
    rd_send[...] = read
    for d in range(1, n_sp):
        read_copy(peer(d), sp, d).start()

    raw = read + jnp.sum(
        q * new_key[...].astype(jnp.float32), axis=-1, keepdims=True
    ) * new_value[...].astype(jnp.float32)
    for d in range(1, n_sp):
        read_copy(peer(d), peer(d), d).wait_recv()
        raw += rd_recv[peer(d)]
    scale = lax.rsqrt(jnp.mean(raw * raw, axis=-1, keepdims=True) + norm_epsilon)
    read_out[...] = (raw * scale * gain[...]).astype(jnp.bfloat16)

    state = st_send[sp]
    for d in range(1, n_sp):
        state_copy(peer(d), peer(d), d).wait_recv()
        state += st_recv[peer(d)]
    state_out[...] = state.astype(jnp.bfloat16)

    def drain(c, carry):
        for j in range(len(bits)):
            own_copy(c, j).wait_send()
        for n in range(len(relays)):
            relay_copy(c, n).wait_send()
        return carry

    lax.fori_loop(0, chunks, drain, 0)
    for d in range(1, n_sp):
        total_copy(d).wait_send()
        state_copy(peer(d), sp, d).wait_send()
        read_copy(peer(d), sp, d).wait_send()


def shards(
    n_sp,
    n_tp,
    tokens,
    key_weight,
    value_weight,
    decay_weight,
    decay_bias,
    decay_shift,
    new_query,
    new_key,
    new_value,
    out_gain,
):
    t_count, feat = tokens.shape
    depth, width = key_weight.shape
    v_width = value_weight.shape[1]
    heads = width // DK
    r_count = DK // n_sp
    rows = min(CHUNK, t_count)
    chunks = t_count // rows
    n_bits = n_tp.bit_length() - 1
    n_relays = n_tp * n_tp
    any_spec = pl.BlockSpec(memory_space=pl.ANY)
    vmem_spec = pl.BlockSpec(memory_space=pltpu.VMEM)
    dma = pltpu.SemaphoreType.DMA
    f32, bf16 = jnp.float32, jnp.bfloat16
    return pl.pallas_call(
        functools.partial(kernel, n_sp, n_tp),
        out_shape=(
            jax.ShapeDtypeStruct((2, heads, r_count, DV), bf16),
            jax.ShapeDtypeStruct((heads, DV), bf16),
        ),
        in_specs=[any_spec] * 4 + [vmem_spec] * 6,
        out_specs=(vmem_spec, vmem_spec),
        scratch_shapes=[
            pltpu.VMEM((n_tp, t_count, feat), bf16),
            pltpu.VMEM((depth, width), bf16),
            pltpu.VMEM((depth, v_width), bf16),
            pltpu.VMEM((2, depth, width), bf16),
            pltpu.VMEM((2, rows, width), f32),
            pltpu.VMEM((2, rows, v_width), f32),
            pltpu.VMEM((2, 2, rows, width), f32),
            pltpu.VMEM((DV, width), f32),
            pltpu.VMEM((DV, width), f32),
            pltpu.VMEM((2, width), f32),
            pltpu.VMEM((n_sp, 2, width), f32),
            pltpu.VMEM((n_sp, 2, heads, r_count, DV), f32),
            pltpu.VMEM((n_sp, 2, heads, r_count, DV), f32),
            pltpu.VMEM((heads, DV), f32),
            pltpu.VMEM((n_sp, heads, DV), f32),
            dma((1,)),
            dma((n_tp, 4)),
            dma((max(n_bits, 1), chunks)),
            dma((n_relays, chunks)),
            dma((n_tp, chunks, 2)),
            dma((n_sp,)),
            dma((n_sp,)),
            dma((n_sp,)),
            dma((n_sp,)),
            dma((n_sp,)),
            dma((n_sp,)),
        ],
        compiler_params=pltpu.CompilerParams(collective_id=0, has_side_effects=True),
    )(
        tokens,
        key_weight,
        value_weight,
        decay_weight,
        decay_bias,
        decay_shift,
        new_query,
        new_key,
        new_value,
        out_gain.reshape(1, DV),
    )


def solution(mesh):
    placed = (
        P("sp", "tp"),
        P(None, "tp"),
        P(None, "tp"),
        P(None, None, "tp"),
        P(None, "tp"),
        P("sp", "tp"),
        P("tp", None),
        P("tp", None),
        P("tp", None),
        P(),
    )
    return jax.shard_map(
        functools.partial(shards, mesh.shape["sp"], mesh.shape["tp"]),
        mesh=mesh,
        in_specs=placed,
        out_specs=(P(None, "tp", "sp", None), P("tp", None)),
        check_vma=False,
    )
```

```python
import functools

import jax
import jax.numpy as jnp
from jax import lax
from jax.experimental import pallas as pl
from jax.experimental.pallas import tpu as pltpu
from jax.sharding import PartitionSpec as P

DK = 64
DV = 128
CHUNK = 128

gate_norm = 16.0
norm_epsilon = 1e-06

MESH = pl.DeviceIdType.MESH


def flipped(index, bits, d):
    out = index
    for b in bits:
        if d & b:
            out = out + b - 2 * b * lax.rem(lax.div(index, b), 2)
    return out


def kernel(
    n_sp,
    n_tp,
    tokens,
    kw,
    vw,
    dw,
    bias_in,
    shift_in,
    query_in,
    new_key_in,
    new_value_in,
    gain_in,
    state_out,
    read_out,
    bias,
    shift,
    query,
    new_key,
    new_value,
    gain,
    state_buf,
    read_buf,
    tok_buf,
    kw_buf,
    vw_buf,
    dw_buf,
    acc_k,
    acc_v,
    acc_d,
    s_fwd,
    s_bwd,
    tot_own,
    tot_buf,
    st_own,
    st_send,
    st_recv,
    rd_send,
    rd_recv,
    local_sem,
    w_sem,
    own_send_sem,
    relay_send_sem,
    recv_sem,
    tot_send_sem,
    tot_recv_sem,
    st_send_sem,
    st_recv_sem,
    rd_send_sem,
    rd_recv_sem,
):
    sp = lax.axis_index("sp")
    tp = lax.axis_index("tp")
    bits = [1 << i for i in range(n_tp.bit_length() - 1)]
    order = sorted(range(n_tp), key=lambda d: (bin(d).count("1"), d))
    level = [bin(d).count("1") for d in order]
    place = {d: i for i, d in enumerate(order)}
    direct = [i for i in range(n_tp) if level[i] == 1]
    near = sum(1 for lv in level if lv <= 1)

    t_count, feat = tokens.shape
    rows = min(CHUNK, t_count)
    half = rows // 2
    chunks = t_count // rows
    width = kw.shape[1]
    heads = width // DK
    pair = 2 if heads % 2 == 0 else 1
    groups = heads // pair
    lanes = pair * DK
    r_count = DK // n_sp

    local = []
    for i, d in enumerate(order):
        src = pl.ds(pl.multiple_of(flipped(tp, bits, d) * feat, feat), feat)
        dst = pl.ds(i * feat, feat)
        local.append(pltpu.make_async_copy(kw.at[src], kw_buf.at[dst], w_sem.at[i, 0]))
        local.append(pltpu.make_async_copy(vw.at[src], vw_buf.at[dst], w_sem.at[i, 1]))
        for k in range(2):
            local.append(
                pltpu.make_async_copy(dw.at[k, src], dw_buf.at[k, dst], w_sem.at[i, 2 + k])
            )
    local.append(pltpu.make_async_copy(tokens, tok_buf.at[0], local_sem.at[0]))
    small = (
        (bias_in, bias),
        (shift_in, shift),
        (query_in, query),
        (new_key_in, new_key),
        (new_value_in, new_value),
        (gain_in, gain),
    )
    for n, (src, dst) in enumerate(small):
        local.append(pltpu.make_async_copy(src, dst, local_sem.at[1 + n]))
    read_done = pltpu.make_async_copy(read_buf, read_out, local_sem.at[7])
    state_done = pltpu.make_async_copy(state_buf, state_out, local_sem.at[8])

    barrier = pltpu.get_barrier_semaphore()
    for b in bits:
        pl.semaphore_signal(
            barrier, inc=1, device_id=(sp, flipped(tp, bits, b)), device_id_type=MESH
        )
    for d in range(1, n_sp):
        pl.semaphore_signal(
            barrier, inc=1, device_id=(lax.rem(sp + d, n_sp), tp), device_id_type=MESH
        )
    pl.semaphore_wait(barrier, len(bits) + n_sp - 1)

    def part(c, h):
        if h is None:
            return pl.ds(pl.multiple_of(c * rows, rows), rows)
        return pl.ds(pl.multiple_of(c * rows + h * half, half), half)

    def own_copy(c, j):
        b = bits[j]
        rs = part(c, None)
        return pltpu.make_async_remote_copy(
            src_ref=tokens.at[rs],
            dst_ref=tok_buf.at[place[b], rs],
            send_sem=own_send_sem.at[j, c],
            recv_sem=recv_sem.at[place[b], c, 0],
            device_id=(sp, flipped(tp, bits, b)),
            device_id_type=MESH,
        )

    relays = []
    for d in order[1:]:
        for b in bits:
            if not d & b:
                if b > d:
                    relays.append((d, 0, b))
                if all(b < o for o in bits if d & o):
                    relays.append((d, 1, b))

    def relay_copy(c, n):
        d, h, b = relays[n]
        rs = part(c, h)
        return pltpu.make_async_remote_copy(
            src_ref=tok_buf.at[place[d], rs],
            dst_ref=tok_buf.at[place[d | b], rs],
            send_sem=relay_send_sem.at[n, c],
            recv_sem=recv_sem.at[place[d | b], c, h],
            device_id=(sp, flipped(tp, bits, b)),
            device_id_type=MESH,
        )

    def send_own(c):
        for j in range(len(bits)):
            own_copy(c, j).start()

    def wait_direct(c):
        for j in range(len(bits)):
            own_copy(c, j).wait_recv()

    def relay_level(c, lv):
        for n, (d, h, b) in enumerate(relays):
            if bin(d).count("1") == lv:
                relay_copy(c, n).start()

    def wait_level(c, lv):
        for n, (d, h, b) in enumerate(relays):
            if bin(d | b).count("1") == lv:
                relay_copy(c, n).wait_recv()

    for c in range(min(2, chunks)):
        send_own(c)
    for copy in local:
        copy.start()

    s_fwd[...] = jnp.zeros_like(s_fwd)
    s_bwd[...] = jnp.zeros_like(s_bwd)
    tot_own[...] = jnp.zeros_like(tot_own)

    t_ids = lax.broadcasted_iota(jnp.int32, (rows, 2 * rows), 0)
    s_ids = lax.broadcasted_iota(jnp.int32, (rows, 2 * rows), 1)
    s_ids = jnp.where(s_ids >= rows, s_ids - rows, s_ids)
    after = jnp.where(s_ids > t_ids, 1.0, 0.0).astype(jnp.bfloat16)
    before = jnp.where(s_ids < t_ids, 1.0, 0.0).astype(jnp.bfloat16)
    first_head = lax.broadcasted_iota(jnp.int32, (DV, lanes), 1) < DK
    first_head_rows = lax.broadcasted_iota(jnp.int32, (rows, lanes), 1) < DK

    def dot(a, b):
        return jnp.dot(a, b, preferred_element_type=jnp.float32)

    def product(c, low, high):
        rs = part(c, None)
        x = jnp.concatenate([tok_buf[i, rs, :] for i in range(low, high)], axis=1)
        ws = slice(low * feat, high * feat)
        return (
            dot(x, kw_buf[ws, :]),
            dot(x, vw_buf[ws, :]),
            dot(x, dw_buf[0, ws, :]),
            dot(x, dw_buf[1, ws, :]),
        )

    def begin(c):
        p = lax.rem(c, 2)
        k, v, f, b = product(c, 0, near)
        acc_k[p] = k
        acc_v[p] = v
        acc_d[p, 0] = f
        acc_d[p, 1] = b

    def log_gate(pre, shift_wide):
        return (
            jnp.minimum(pre, 0.0) - jnp.log(1.0 + jnp.exp(-jnp.abs(pre)))
        ) * (1.0 / gate_norm) + shift_wide

    def summed(mask, log):
        hi = log.astype(jnp.bfloat16)
        lo = (log - hi.astype(jnp.float32)).astype(jnp.bfloat16)
        return dot(mask, jnp.concatenate([hi, lo], axis=0))

    def finish(c):
        p = lax.rem(c, 2)
        for lv in range(2, len(bits) + 1):
            wait_level(c, lv)
            relay_level(c, lv)
        k, v, f, b = acc_k[p], acc_v[p], acc_d[p, 0], acc_d[p, 1]
        if near < n_tp:
            more = product(c, near, n_tp)
            k, v, f, b = k + more[0], v + more[1], f + more[2], b + more[3]
        k = k.astype(jnp.bfloat16).astype(jnp.float32)
        v = v.astype(jnp.bfloat16)
        sh = shift[:, part(c, None)].T
        wide = []
        for g in range(groups):
            one = jnp.broadcast_to(sh[:, g * pair : g * pair + 1], (rows, lanes))
            if pair == 2:
                two = jnp.broadcast_to(sh[:, g * pair + 1 : g * pair + 2], (rows, lanes))
                one = jnp.where(first_head_rows, one, two)
            wide.append(one)
        shift_wide = wide[0] if groups == 1 else jnp.concatenate(wide, axis=1)
        f_log = log_gate(f + bias[0:1, :], shift_wide)
        b_log = log_gate(b + bias[1:2, :], shift_wide)
        f_total = jnp.sum(f_log, axis=0, keepdims=True)
        b_total = jnp.sum(b_log, axis=0, keepdims=True)
        f_keys = (k * jnp.exp(summed(after, f_log))).astype(jnp.bfloat16)
        b_keys = (k * jnp.exp(summed(before, b_log) + tot_own[1:2, :])).astype(jnp.bfloat16)
        f_scale = jnp.exp(f_total)
        tot_own[0:1, :] += f_total
        tot_own[1:2, :] += b_total

        def outer(v_group, keys):
            r = lax.dot_general(
                v_group, keys, (((0,), (0,)), ((), ())), preferred_element_type=jnp.float32
            )
            return jnp.where(first_head, r[:DV], r[DV:]) if pair == 2 else r

        for g in range(groups):
            cs = slice(g * lanes, (g + 1) * lanes)
            v_group = v[:, g * pair * DV : (g + 1) * pair * DV]
            s_fwd[:, cs] = s_fwd[:, cs] * f_scale[:, cs] + outer(v_group, f_keys[:, cs])
            s_bwd[:, cs] += outer(v_group, b_keys[:, cs])

    for copy in local:
        copy.wait()

    def step(c, carry):
        wait_direct(c)
        relay_level(c, 1)

        @pl.when(c + 2 < chunks)
        def _():
            send_own(c + 2)

        begin(c)

        @pl.when(c > 0)
        def _():
            finish(c - 1)

        return carry

    lax.fori_loop(0, chunks, step, 0)
    finish(chunks - 1)

    def peer(d):
        return lax.rem(sp + d, n_sp)

    def total_copy(d):
        return pltpu.make_async_remote_copy(
            src_ref=tot_own,
            dst_ref=tot_buf.at[sp],
            send_sem=tot_send_sem.at[d],
            recv_sem=tot_recv_sem.at[sp],
            device_id=(peer(d), tp),
            device_id_type=MESH,
        )

    for d in range(1, n_sp):
        total_copy(d).start()
    later = jnp.zeros((1, width), jnp.float32)
    earlier = jnp.zeros((1, width), jnp.float32)
    for d in range(1, n_sp):
        src = peer(d)
        pltpu.make_async_remote_copy(
            src_ref=tot_own,
            dst_ref=tot_buf.at[src],
            send_sem=tot_send_sem.at[d],
            recv_sem=tot_recv_sem.at[src],
            device_id=(src, tp),
            device_id_type=MESH,
        ).wait_recv()
        got = tot_buf[src]
        later += jnp.where(src > sp, got[0:1, :], 0.0)
        earlier += jnp.where(src < sp, got[1:2, :], 0.0)

    def upright(s):
        tiles = [s[:, g * lanes : (g + 1) * lanes].T for g in range(groups)]
        return tiles[0] if groups == 1 else jnp.concatenate(tiles, axis=0)

    w_fwd = upright(s_fwd[...] * jnp.exp(later))
    w_bwd = upright(s_bwd[...] * jnp.exp(earlier))
    for r in range(n_sp):
        for h in range(heads):
            rs = slice(h * DK + r * r_count, h * DK + (r + 1) * r_count)
            st_send[r, 0, h] = w_fwd[rs].astype(jnp.bfloat16)
            st_send[r, 1, h] = w_bwd[rs].astype(jnp.bfloat16)
            st_own[r, 0, h] = w_fwd[rs]
            st_own[r, 1, h] = w_bwd[rs]

    def state_copy(dst, slot, d):
        return pltpu.make_async_remote_copy(
            src_ref=st_send.at[dst],
            dst_ref=st_recv.at[slot],
            send_sem=st_send_sem.at[d],
            recv_sem=st_recv_sem.at[slot],
            device_id=(dst, tp),
            device_id_type=MESH,
        )

    def read_copy(dst, slot, d):
        return pltpu.make_async_remote_copy(
            src_ref=rd_send,
            dst_ref=rd_recv.at[slot],
            send_sem=rd_send_sem.at[d],
            recv_sem=rd_recv_sem.at[slot],
            device_id=(dst, tp),
            device_id_type=MESH,
        )

    for d in range(1, n_sp):
        state_copy(peer(d), sp, d).start()

    q = query[...].astype(jnp.float32)
    both = w_fwd + w_bwd
    head_ids = lax.broadcasted_iota(jnp.int32, (heads, DV), 0)
    read = jnp.zeros((heads, DV), jnp.float32)
    for h in range(heads):
        one = jnp.dot(
            q,
            both[h * DK : (h + 1) * DK],
            precision=lax.Precision.HIGHEST,
            preferred_element_type=jnp.float32,
        )
        read = jnp.where(head_ids == h, one, read)
    rd_send[...] = read
    for d in range(1, n_sp):
        read_copy(peer(d), sp, d).start()

    raw = read + jnp.sum(
        q * new_key[...].astype(jnp.float32), axis=-1, keepdims=True
    ) * new_value[...].astype(jnp.float32)
    for d in range(1, n_sp):
        read_copy(peer(d), peer(d), d).wait_recv()
        raw += rd_recv[peer(d)]
    scale = lax.rsqrt(jnp.mean(raw * raw, axis=-1, keepdims=True) + norm_epsilon)
    read_buf[...] = (raw * scale * gain[...]).astype(jnp.bfloat16)
    read_done.start()

    state = st_own[sp]
    for d in range(1, n_sp):
        state_copy(peer(d), peer(d), d).wait_recv()
        state += st_recv[peer(d)].astype(jnp.float32)
    state_buf[...] = state.astype(jnp.bfloat16)
    state_done.start()

    def drain(c, carry):
        for j in range(len(bits)):
            own_copy(c, j).wait_send()
        for n in range(len(relays)):
            relay_copy(c, n).wait_send()
        return carry

    lax.fori_loop(0, chunks, drain, 0)
    for d in range(1, n_sp):
        total_copy(d).wait_send()
        state_copy(peer(d), sp, d).wait_send()
        read_copy(peer(d), sp, d).wait_send()
    read_done.wait()
    state_done.wait()


def shards(
    n_sp,
    n_tp,
    tokens,
    key_weight,
    value_weight,
    decay_weight,
    decay_bias,
    decay_shift,
    new_query,
    new_key,
    new_value,
    out_gain,
):
    t_count, feat = tokens.shape
    depth, width = key_weight.shape
    v_width = value_weight.shape[1]
    heads = width // DK
    r_count = DK // n_sp
    rows = min(CHUNK, t_count)
    chunks = t_count // rows
    n_bits = n_tp.bit_length() - 1
    n_relays = n_tp * n_tp
    any_spec = pl.BlockSpec(memory_space=pl.ANY)
    dma = pltpu.SemaphoreType.DMA
    f32, bf16 = jnp.float32, jnp.bfloat16
    return pl.pallas_call(
        functools.partial(kernel, n_sp, n_tp),
        out_shape=(
            jax.ShapeDtypeStruct((2, heads, r_count, DV), bf16),
            jax.ShapeDtypeStruct((heads, DV), bf16),
        ),
        in_specs=[any_spec] * 10,
        out_specs=(any_spec, any_spec),
        scratch_shapes=[
            pltpu.VMEM((2, width), f32),
            pltpu.VMEM((heads, t_count), f32),
            pltpu.VMEM((heads, DK), bf16),
            pltpu.VMEM((heads, DK), bf16),
            pltpu.VMEM((heads, DV), bf16),
            pltpu.VMEM((1, DV), f32),
            pltpu.VMEM((2, heads, r_count, DV), bf16),
            pltpu.VMEM((heads, DV), bf16),
            pltpu.VMEM((n_tp, t_count, feat), bf16),
            pltpu.VMEM((depth, width), bf16),
            pltpu.VMEM((depth, v_width), bf16),
            pltpu.VMEM((2, depth, width), bf16),
            pltpu.VMEM((2, rows, width), f32),
            pltpu.VMEM((2, rows, v_width), f32),
            pltpu.VMEM((2, 2, rows, width), f32),
            pltpu.VMEM((DV, width), f32),
            pltpu.VMEM((DV, width), f32),
            pltpu.VMEM((2, width), f32),
            pltpu.VMEM((n_sp, 2, width), f32),
            pltpu.VMEM((n_sp, 2, heads, r_count, DV), f32),
            pltpu.VMEM((n_sp, 2, heads, r_count, DV), bf16),
            pltpu.VMEM((n_sp, 2, heads, r_count, DV), bf16),
            pltpu.VMEM((heads, DV), f32),
            pltpu.VMEM((n_sp, heads, DV), f32),
            dma((9,)),
            dma((n_tp, 4)),
            dma((max(n_bits, 1), chunks)),
            dma((n_relays, chunks)),
            dma((n_tp, chunks, 2)),
            dma((n_sp,)),
            dma((n_sp,)),
            dma((n_sp,)),
            dma((n_sp,)),
            dma((n_sp,)),
            dma((n_sp,)),
        ],
        compiler_params=pltpu.CompilerParams(collective_id=0, has_side_effects=True),
    )(
        tokens,
        key_weight,
        value_weight,
        decay_weight,
        decay_bias,
        decay_shift.T,
        new_query,
        new_key,
        new_value,
        out_gain.reshape(1, DV),
    )


def solution(mesh):
    placed = (
        P("sp", "tp"),
        P(None, "tp"),
        P(None, "tp"),
        P(None, None, "tp"),
        P(None, "tp"),
        P("sp", "tp"),
        P("tp", None),
        P("tp", None),
        P("tp", None),
        P(),
    )
    return jax.shard_map(
        functools.partial(shards, mesh.shape["sp"], mesh.shape["tp"]),
        mesh=mesh,
        in_specs=placed,
        out_specs=(P(None, "tp", "sp", None), P("tp", None)),
        check_vma=False,
    )
```

```python
import functools

import jax
import jax.numpy as jnp
from jax import lax
from jax.experimental import pallas as pl
from jax.experimental.pallas import tpu as pltpu
from jax.sharding import PartitionSpec as P

DK = 64
DV = 128
CHUNK = 128

gate_norm = 16.0
norm_epsilon = 1e-06

MESH = pl.DeviceIdType.MESH


def flipped(index, bits, d):
    out = index
    for b in bits:
        if d & b:
            out = out + b - 2 * b * lax.rem(lax.div(index, b), 2)
    return out


def kernel(
    n_sp,
    n_tp,
    tokens,
    kw,
    vw,
    dw,
    bias_in,
    shift_in,
    query_in,
    new_key_in,
    new_value_in,
    gain_in,
    state_out,
    read_out,
    bias,
    shift,
    query,
    new_key,
    new_value,
    gain,
    state_buf,
    read_buf,
    tok_buf,
    kw_buf,
    vw_buf,
    dw_buf,
    acc_k,
    acc_v,
    acc_d,
    s_fwd,
    s_bwd,
    tot_own,
    tot_buf,
    st_own,
    st_send,
    st_recv,
    rd_send,
    rd_recv,
    local_sem,
    w_sem,
    own_send_sem,
    relay_send_sem,
    recv_sem,
    tot_send_sem,
    tot_recv_sem,
    st_send_sem,
    st_recv_sem,
    rd_send_sem,
    rd_recv_sem,
    up_sem,
    down_sem,
    pair_sem,
):
    sp = lax.axis_index("sp")
    tp = lax.axis_index("tp")
    bits = [1 << i for i in range(n_tp.bit_length() - 1)]
    order = sorted(range(n_tp), key=lambda d: (bin(d).count("1"), d))
    level = [bin(d).count("1") for d in order]
    place = {d: i for i, d in enumerate(order)}
    direct = [i for i in range(n_tp) if level[i] == 1]
    near = sum(1 for lv in level if lv <= 1)

    t_count, feat = tokens.shape
    rows = min(CHUNK, t_count)
    half = rows // 2
    chunks = t_count // rows
    width = kw.shape[1]
    heads = width // DK
    pair = 2 if heads % 2 == 0 else 1
    groups = heads // pair
    lanes = pair * DK
    r_count = DK // n_sp

    local = []
    for i, d in enumerate(order):
        src = pl.ds(pl.multiple_of(flipped(tp, bits, d) * feat, feat), feat)
        dst = pl.ds(i * feat, feat)
        local.append(pltpu.make_async_copy(kw.at[src], kw_buf.at[dst], w_sem.at[i, 0]))
        local.append(pltpu.make_async_copy(vw.at[src], vw_buf.at[dst], w_sem.at[i, 1]))
        for k in range(2):
            local.append(
                pltpu.make_async_copy(dw.at[k, src], dw_buf.at[k, dst], w_sem.at[i, 2 + k])
            )
    local.append(pltpu.make_async_copy(tokens, tok_buf.at[0], local_sem.at[0]))
    small = (
        (bias_in, bias),
        (shift_in, shift),
        (query_in, query),
        (new_key_in, new_key),
        (new_value_in, new_value),
        (gain_in, gain),
    )
    for n, (src, dst) in enumerate(small):
        local.append(pltpu.make_async_copy(src, dst, local_sem.at[1 + n]))
    read_done = pltpu.make_async_copy(read_buf, read_out, local_sem.at[7])
    state_done = pltpu.make_async_copy(state_buf, state_out, local_sem.at[8])

    barrier = pltpu.get_barrier_semaphore()
    for b in bits:
        pl.semaphore_signal(
            barrier, inc=1, device_id=(sp, flipped(tp, bits, b)), device_id_type=MESH
        )
    z_count = n_sp // 2
    z = lax.div(sp, 2)
    partner = sp + 1 - 2 * lax.rem(sp, 2)
    pl.semaphore_signal(barrier, inc=1, device_id=(partner, tp), device_id_type=MESH)

    def signal_if(condition, sem, target):
        @pl.when(condition)
        def _():
            pl.semaphore_signal(sem, inc=1, device_id=(target, tp), device_id_type=MESH)

    def wait_if(condition, sem):
        @pl.when(condition)
        def _():
            pl.semaphore_wait(sem, 1)

    signal_if(z >= 1, barrier, sp - 2)
    signal_if(z + 1 < z_count, barrier, sp + 2)
    ends = jnp.where(z >= 1, 1, 0) + jnp.where(z + 1 < z_count, 1, 0)
    pl.semaphore_wait(barrier, len(bits) + 1 + ends)

    def part(c, h):
        if h is None:
            return pl.ds(pl.multiple_of(c * rows, rows), rows)
        return pl.ds(pl.multiple_of(c * rows + h * half, half), half)

    def own_copy(c, j):
        b = bits[j]
        rs = part(c, None)
        return pltpu.make_async_remote_copy(
            src_ref=tokens.at[rs],
            dst_ref=tok_buf.at[place[b], rs],
            send_sem=own_send_sem.at[j, c],
            recv_sem=recv_sem.at[place[b], c, 0],
            device_id=(sp, flipped(tp, bits, b)),
            device_id_type=MESH,
        )

    relays = []
    for d in order[1:]:
        for b in bits:
            if not d & b:
                if b > d:
                    relays.append((d, 0, b))
                if all(b < o for o in bits if d & o):
                    relays.append((d, 1, b))

    def relay_copy(c, n):
        d, h, b = relays[n]
        rs = part(c, h)
        return pltpu.make_async_remote_copy(
            src_ref=tok_buf.at[place[d], rs],
            dst_ref=tok_buf.at[place[d | b], rs],
            send_sem=relay_send_sem.at[n, c],
            recv_sem=recv_sem.at[place[d | b], c, h],
            device_id=(sp, flipped(tp, bits, b)),
            device_id_type=MESH,
        )

    def send_own(c):
        for j in range(len(bits)):
            own_copy(c, j).start()

    def wait_direct(c):
        for j in range(len(bits)):
            own_copy(c, j).wait_recv()

    def relay_level(c, lv):
        for n, (d, h, b) in enumerate(relays):
            if bin(d).count("1") == lv:
                relay_copy(c, n).start()

    def wait_level(c, lv):
        for n, (d, h, b) in enumerate(relays):
            if bin(d | b).count("1") == lv:
                relay_copy(c, n).wait_recv()

    for c in range(min(2, chunks)):
        send_own(c)
    for copy in local:
        copy.start()

    s_fwd[...] = jnp.zeros_like(s_fwd)
    s_bwd[...] = jnp.zeros_like(s_bwd)
    tot_own[...] = jnp.zeros_like(tot_own)

    t_ids = lax.broadcasted_iota(jnp.int32, (rows, 2 * rows), 0)
    s_ids = lax.broadcasted_iota(jnp.int32, (rows, 2 * rows), 1)
    s_ids = jnp.where(s_ids >= rows, s_ids - rows, s_ids)
    after = jnp.where(s_ids > t_ids, 1.0, 0.0).astype(jnp.bfloat16)
    before = jnp.where(s_ids < t_ids, 1.0, 0.0).astype(jnp.bfloat16)
    first_head = lax.broadcasted_iota(jnp.int32, (DV, lanes), 1) < DK
    first_head_rows = lax.broadcasted_iota(jnp.int32, (rows, lanes), 1) < DK

    def dot(a, b):
        return jnp.dot(a, b, preferred_element_type=jnp.float32)

    def product(c, low, high):
        rs = part(c, None)
        x = jnp.concatenate([tok_buf[i, rs, :] for i in range(low, high)], axis=1)
        ws = slice(low * feat, high * feat)
        return (
            dot(x, kw_buf[ws, :]),
            dot(x, vw_buf[ws, :]),
            dot(x, dw_buf[0, ws, :]),
            dot(x, dw_buf[1, ws, :]),
        )

    def begin(c):
        p = lax.rem(c, 2)
        k, v, f, b = product(c, 0, near)
        acc_k[p] = k
        acc_v[p] = v
        acc_d[p, 0] = f
        acc_d[p, 1] = b

    def log_gate(pre, shift_wide):
        return (
            jnp.minimum(pre, 0.0) - jnp.log(1.0 + jnp.exp(-jnp.abs(pre)))
        ) * (1.0 / gate_norm) + shift_wide

    def summed(mask, log):
        hi = log.astype(jnp.bfloat16)
        lo = (log - hi.astype(jnp.float32)).astype(jnp.bfloat16)
        return dot(mask, jnp.concatenate([hi, lo], axis=0))

    def finish(c):
        p = lax.rem(c, 2)
        for lv in range(2, len(bits) + 1):
            wait_level(c, lv)
            relay_level(c, lv)
        k, v, f, b = acc_k[p], acc_v[p], acc_d[p, 0], acc_d[p, 1]
        if near < n_tp:
            more = product(c, near, n_tp)
            k, v, f, b = k + more[0], v + more[1], f + more[2], b + more[3]
        k = k.astype(jnp.bfloat16).astype(jnp.float32)
        v = v.astype(jnp.bfloat16)
        sh = shift[:, part(c, None)].T
        wide = []
        for g in range(groups):
            one = jnp.broadcast_to(sh[:, g * pair : g * pair + 1], (rows, lanes))
            if pair == 2:
                two = jnp.broadcast_to(sh[:, g * pair + 1 : g * pair + 2], (rows, lanes))
                one = jnp.where(first_head_rows, one, two)
            wide.append(one)
        shift_wide = wide[0] if groups == 1 else jnp.concatenate(wide, axis=1)
        f_log = log_gate(f + bias[0:1, :], shift_wide)
        b_log = log_gate(b + bias[1:2, :], shift_wide)
        f_total = jnp.sum(f_log, axis=0, keepdims=True)
        b_total = jnp.sum(b_log, axis=0, keepdims=True)
        f_keys = (k * jnp.exp(summed(after, f_log))).astype(jnp.bfloat16)
        b_keys = (k * jnp.exp(summed(before, b_log) + tot_own[1:2, :])).astype(jnp.bfloat16)
        f_scale = jnp.exp(f_total)
        tot_own[0:1, :] += f_total
        tot_own[1:2, :] += b_total

        def outer(v_group, keys):
            r = lax.dot_general(
                v_group, keys, (((0,), (0,)), ((), ())), preferred_element_type=jnp.float32
            )
            return jnp.where(first_head, r[:DV], r[DV:]) if pair == 2 else r

        for g in range(groups):
            cs = slice(g * lanes, (g + 1) * lanes)
            v_group = v[:, g * pair * DV : (g + 1) * pair * DV]
            s_fwd[:, cs] = s_fwd[:, cs] * f_scale[:, cs] + outer(v_group, f_keys[:, cs])
            s_bwd[:, cs] += outer(v_group, b_keys[:, cs])

    for k in range(1, z_count - 1):
        signal_if((z >= 1) & (z + k < z_count), up_sem.at[k], sp - 2)
        signal_if((z + 1 < z_count) & (z >= k), down_sem.at[k], sp + 2)
        wait_if(z + 1 + k < z_count, up_sem.at[k])
        wait_if(z >= 1 + k, down_sem.at[k])
    pl.semaphore_signal(pair_sem, inc=1, device_id=(partner, tp), device_id_type=MESH)
    pl.semaphore_wait(pair_sem, 1)

    for copy in local:
        copy.wait()

    def step(c, carry):
        wait_direct(c)
        relay_level(c, 1)

        @pl.when(c + 2 < chunks)
        def _():
            send_own(c + 2)

        begin(c)

        @pl.when(c > 0)
        def _():
            finish(c - 1)

        return carry

    lax.fori_loop(0, chunks, step, 0)
    finish(chunks - 1)

    def peer(d):
        return lax.rem(sp + d, n_sp)

    def total_copy(d):
        return pltpu.make_async_remote_copy(
            src_ref=tot_own,
            dst_ref=tot_buf.at[sp],
            send_sem=tot_send_sem.at[d],
            recv_sem=tot_recv_sem.at[sp],
            device_id=(peer(d), tp),
            device_id_type=MESH,
        )

    for d in range(1, n_sp):
        total_copy(d).start()
    later = jnp.zeros((1, width), jnp.float32)
    earlier = jnp.zeros((1, width), jnp.float32)
    for d in range(1, n_sp):
        src = peer(d)
        pltpu.make_async_remote_copy(
            src_ref=tot_own,
            dst_ref=tot_buf.at[src],
            send_sem=tot_send_sem.at[d],
            recv_sem=tot_recv_sem.at[src],
            device_id=(src, tp),
            device_id_type=MESH,
        ).wait_recv()
        got = tot_buf[src]
        later += jnp.where(src > sp, got[0:1, :], 0.0)
        earlier += jnp.where(src < sp, got[1:2, :], 0.0)

    def upright(s):
        tiles = [s[:, g * lanes : (g + 1) * lanes].T for g in range(groups)]
        return tiles[0] if groups == 1 else jnp.concatenate(tiles, axis=0)

    w_fwd = upright(s_fwd[...] * jnp.exp(later))
    w_bwd = upright(s_bwd[...] * jnp.exp(earlier))
    for r in range(n_sp):
        for h in range(heads):
            rs = slice(h * DK + r * r_count, h * DK + (r + 1) * r_count)
            st_send[r, 0, h] = w_fwd[rs].astype(jnp.bfloat16)
            st_send[r, 1, h] = w_bwd[rs].astype(jnp.bfloat16)
            st_own[r, 0, h] = w_fwd[rs]
            st_own[r, 1, h] = w_bwd[rs]

    def state_copy(dst, slot, d):
        return pltpu.make_async_remote_copy(
            src_ref=st_send.at[dst],
            dst_ref=st_recv.at[slot],
            send_sem=st_send_sem.at[d],
            recv_sem=st_recv_sem.at[slot],
            device_id=(dst, tp),
            device_id_type=MESH,
        )

    def read_copy(dst, slot, d):
        return pltpu.make_async_remote_copy(
            src_ref=rd_send,
            dst_ref=rd_recv.at[slot],
            send_sem=rd_send_sem.at[d],
            recv_sem=rd_recv_sem.at[slot],
            device_id=(dst, tp),
            device_id_type=MESH,
        )

    for d in range(1, n_sp):
        state_copy(peer(d), sp, d).start()

    q = query[...].astype(jnp.float32)
    both = w_fwd + w_bwd
    head_ids = lax.broadcasted_iota(jnp.int32, (heads, DV), 0)
    read = jnp.zeros((heads, DV), jnp.float32)
    for h in range(heads):
        one = jnp.dot(
            q,
            both[h * DK : (h + 1) * DK],
            precision=lax.Precision.HIGHEST,
            preferred_element_type=jnp.float32,
        )
        read = jnp.where(head_ids == h, one, read)
    rd_send[...] = read
    for d in range(1, n_sp):
        read_copy(peer(d), sp, d).start()

    raw = read + jnp.sum(
        q * new_key[...].astype(jnp.float32), axis=-1, keepdims=True
    ) * new_value[...].astype(jnp.float32)
    for d in range(1, n_sp):
        read_copy(peer(d), peer(d), d).wait_recv()
        raw += rd_recv[peer(d)]
    scale = lax.rsqrt(jnp.mean(raw * raw, axis=-1, keepdims=True) + norm_epsilon)
    read_buf[...] = (raw * scale * gain[...]).astype(jnp.bfloat16)
    read_done.start()

    state = st_own[sp]
    for d in range(1, n_sp):
        state_copy(peer(d), peer(d), d).wait_recv()
        state += st_recv[peer(d)].astype(jnp.float32)
    state_buf[...] = state.astype(jnp.bfloat16)
    state_done.start()

    def drain(c, carry):
        for j in range(len(bits)):
            own_copy(c, j).wait_send()
        for n in range(len(relays)):
            relay_copy(c, n).wait_send()
        return carry

    lax.fori_loop(0, chunks, drain, 0)
    for d in range(1, n_sp):
        total_copy(d).wait_send()
        state_copy(peer(d), sp, d).wait_send()
        read_copy(peer(d), sp, d).wait_send()
    read_done.wait()
    state_done.wait()


def hand_over(state, read):
    def body(state_in, read_in, state_out, read_out):
        state_out[...] = state_in[...]
        read_out[...] = read_in[...]

    vmem_spec = pl.BlockSpec(memory_space=pltpu.VMEM)
    return pl.pallas_call(
        body,
        out_shape=(
            jax.ShapeDtypeStruct(state.shape, state.dtype),
            jax.ShapeDtypeStruct(read.shape, read.dtype),
        ),
        in_specs=[vmem_spec, vmem_spec],
        out_specs=(vmem_spec, vmem_spec),
    )(state, read)


def shards(
    n_sp,
    n_tp,
    tokens,
    key_weight,
    value_weight,
    decay_weight,
    decay_bias,
    decay_shift,
    new_query,
    new_key,
    new_value,
    out_gain,
):
    t_count, feat = tokens.shape
    depth, width = key_weight.shape
    v_width = value_weight.shape[1]
    heads = width // DK
    r_count = DK // n_sp
    rows = min(CHUNK, t_count)
    chunks = t_count // rows
    n_bits = n_tp.bit_length() - 1
    n_relays = n_tp * n_tp
    any_spec = pl.BlockSpec(memory_space=pl.ANY)
    dma = pltpu.SemaphoreType.DMA
    f32, bf16 = jnp.float32, jnp.bfloat16
    results = pl.pallas_call(
        functools.partial(kernel, n_sp, n_tp),
        out_shape=(
            jax.ShapeDtypeStruct((2, heads, r_count, DV), bf16),
            jax.ShapeDtypeStruct((heads, DV), bf16),
        ),
        in_specs=[any_spec] * 10,
        out_specs=(any_spec, any_spec),
        scratch_shapes=[
            pltpu.VMEM((2, width), f32),
            pltpu.VMEM((heads, t_count), f32),
            pltpu.VMEM((heads, DK), bf16),
            pltpu.VMEM((heads, DK), bf16),
            pltpu.VMEM((heads, DV), bf16),
            pltpu.VMEM((1, DV), f32),
            pltpu.VMEM((2, heads, r_count, DV), bf16),
            pltpu.VMEM((heads, DV), bf16),
            pltpu.VMEM((n_tp, t_count, feat), bf16),
            pltpu.VMEM((depth, width), bf16),
            pltpu.VMEM((depth, v_width), bf16),
            pltpu.VMEM((2, depth, width), bf16),
            pltpu.VMEM((2, rows, width), f32),
            pltpu.VMEM((2, rows, v_width), f32),
            pltpu.VMEM((2, 2, rows, width), f32),
            pltpu.VMEM((DV, width), f32),
            pltpu.VMEM((DV, width), f32),
            pltpu.VMEM((2, width), f32),
            pltpu.VMEM((n_sp, 2, width), f32),
            pltpu.VMEM((n_sp, 2, heads, r_count, DV), f32),
            pltpu.VMEM((n_sp, 2, heads, r_count, DV), bf16),
            pltpu.VMEM((n_sp, 2, heads, r_count, DV), bf16),
            pltpu.VMEM((heads, DV), f32),
            pltpu.VMEM((n_sp, heads, DV), f32),
            dma((9,)),
            dma((n_tp, 4)),
            dma((max(n_bits, 1), chunks)),
            dma((n_relays, chunks)),
            dma((n_tp, chunks, 2)),
            dma((n_sp,)),
            dma((n_sp,)),
            dma((n_sp,)),
            dma((n_sp,)),
            dma((n_sp,)),
            dma((n_sp,)),
            pltpu.SemaphoreType.REGULAR((n_sp,)),
            pltpu.SemaphoreType.REGULAR((n_sp,)),
            pltpu.SemaphoreType.REGULAR,
        ],
        compiler_params=pltpu.CompilerParams(collective_id=0, has_side_effects=True),
    )(
        tokens,
        key_weight,
        value_weight,
        decay_weight,
        decay_bias,
        decay_shift.T,
        new_query,
        new_key,
        new_value,
        out_gain.reshape(1, DV),
    )
    return hand_over(*results)


def solution(mesh):
    placed = (
        P("sp", "tp"),
        P(None, "tp"),
        P(None, "tp"),
        P(None, None, "tp"),
        P(None, "tp"),
        P("sp", "tp"),
        P("tp", None),
        P("tp", None),
        P("tp", None),
        P(),
    )
    return jax.shard_map(
        functools.partial(shards, mesh.shape["sp"], mesh.shape["tp"]),
        mesh=mesh,
        in_specs=placed,
        out_specs=(P(None, "tp", "sp", None), P("tp", None)),
        check_vma=False,
    )
```
